32 devices in a mesh: vp: 8 (over z, x), dp: 4 (over y, core).
Axes of the slice: x: 2, y: 2, z: 4, core: 2. Of those that a mesh axis runs over, the one named last changes fastest.
Arguments:
- stream: bfloat16 [1024, 2048], P(('dp', 'vp')), may hold values from -60 to 60
- hidden: bfloat16 [1024, 5632], P('dp', 'vp'), may hold values from -6 to 6
- w_down: bfloat16 [5632, 2048], P(None, 'vp'), may hold values from -0.078125 to 0.078125
- final_gain: float32 [2048], replicated, may hold values from 0.1 to 1.9
- vocab: bfloat16 [2048, 32768], P(None, 'vp'), may hold values from -2 to 200
- vocab_bias: float32 [32768], P('vp'), may hold values from -5 to 5
- targets: int32 [1024], P('dp'), may hold values from 0 to 32767
Outputs:
- losses: float32 [1024], P(('dp', 'vp'))
- grad_input: float32 [1024, 2048], P(('dp', 'vp'))
- grad_vocab: float32 [2048, 32768], P('dp', 'vp')
The draws below stay inside these ranges and needn't reach their ends.
All inputs are finite; a program needn't handle non-finite values.
Results may differ from the reference program's by a relative error of at most 0.02.
Values may be sent and summed in bfloat16 or wider, within the bound.
A program may use at most 128 MiB of HBM per device.

```python
import math
import jax
import jax.numpy as jnp
import numpy as np
from jax import lax

D = 2048
FF = 5632
VOCAB = 32768
TOK_GROUP = 256
TOKENS = 1024
COLS_DEV = 4096


def draw_stream(key, part):
    ramp = 3.0 ** (jnp.arange(D, dtype=jnp.float32) / (D - 1))
    base = jnp.clip(jax.random.normal(key, (TOKENS, D), jnp.float32), -6.0, 6.0)
    values = base * ramp
    return values.astype(jnp.bfloat16)


def draw_vocab(key, part):
    base = jnp.clip(jax.random.normal(key, (D, VOCAB), jnp.float32), -6.0, 6.0) * (2.5 / math.sqrt(D))
    return base.astype(jnp.bfloat16)


def draw_vocab_bias(key, part):
    shards = VOCAB // COLS_DEV
    shard = (jnp.arange(VOCAB, dtype=jnp.int32) // COLS_DEV).astype(jnp.float32)
    ramp = 2.0 * shard / max(shards - 1, 1) - 1.0
    noise = jnp.clip(jax.random.normal(key, (VOCAB,), jnp.float32), -4.0, 4.0)
    return 0.5 * noise + ramp


def with_ends(result, own_key, least, largest):
    place = [jax.random.randint(jax.random.fold_in(own_key, axis), (), 0, length) for axis, length in enumerate(result.shape)]
    widest = result.shape.index(max(result.shape))
    next_to = place[:widest] + [(place[widest] + 1) % result.shape[widest]] + place[widest + 1:]
    return result.at[tuple(place)].set(least).at[tuple(next_to)].set(largest)


def steps_of(key, shape, cuts, low, high):
    gain, own = 1.0, jax.random.fold_in(key, 6)
    for position, shards_of in cuts:
        draws = jnp.exp(jax.random.uniform(jax.random.fold_in(own, position), (shards_of,), jnp.float32, low / len(cuts), high / len(cuts)))
        gain = gain * jnp.repeat(draws, shape[position] // shards_of).reshape([-1 if axis == position else 1 for axis in range(len(shape))])
    return gain


def rank_table(amount, lean):
    portions = [(1 << 20) // math.isqrt(standing ** lean) + 1 for standing in range(1, amount + 1)]
    width = 1 + sum(portions) // (1 << 30)
    return np.cumsum(np.array([max(1, weight // width) for weight in portions]))


def ranked_ids(own_key, dims, count, lean):
    listing = rank_table(count, lean)
    pick = jax.random.randint(jax.random.fold_in(own_key, 1), dims, 0, int(listing[count - 1]))
    standing = jnp.searchsorted(jnp.asarray(listing, jnp.int32), pick, side="right")
    return jax.random.permutation(jax.random.fold_in(own_key, 2), count)[standing].astype(jnp.int32)


def centred(own_key, dims, deviation, reach, split=(), kind=jnp.bfloat16):
    result = deviation * jax.random.normal(own_key, dims, jnp.float32)
    if split:
        result = result * steps_of(own_key, dims, split, -0.22, 0.18)
    return jnp.clip(result, -reach, reach).astype(kind)


def setup_inputs(seed: int = 0) -> dict:
    key_list = jax.random.split(jax.random.key(seed), 8)
    return {
        "stream": draw_stream(jax.random.fold_in(key_list[7], 71), 0),
        "hidden": centred(key_list[1], (TOKENS, FF), 1.0, 6.0, ((0, 4), (1, 8))),
        "w_down": centred(key_list[2], (FF, D), FF ** -0.5, 0.078125, ((1, 8),)),
        "final_gain": jnp.clip(1.0 + 0.18 * jax.random.normal(key_list[3], (D,), jnp.float32), 0.1, 1.9),
        "vocab": draw_vocab(jax.random.fold_in(key_list[7], 71), 0),
        "vocab_bias": draw_vocab_bias(jax.random.fold_in(key_list[7], 71), 0),
        "targets": with_ends(ranked_ids(key_list[6], (TOKENS,), VOCAB, 2), jax.random.fold_in(key_list[6], 3), 0, VOCAB - 1).astype(jnp.int32),
    }


norm_eps = 1e-06
zloss_weight = 0.001

def reference(stream, hidden, w_down, final_gain, vocab, vocab_bias, targets):
    proj = jnp.dot(hidden, w_down, preferred_element_type=jnp.float32)
    normin = (stream.astype(jnp.float32) + proj).astype(jnp.bfloat16)
    values = normin.astype(jnp.float32)
    inv = lax.rsqrt(lax.optimization_barrier(jnp.mean(values * values, axis=1, keepdims=True)) + norm_eps)
    normed = (values * inv * final_gain).astype(jnp.bfloat16)
    groups = TOKENS // TOK_GROUP
    normed_blocks = normed.reshape(groups, TOK_GROUP, D)
    target_blocks = targets.reshape(groups, TOK_GROUP)

    def one_group(carry, inputs):
        rows, goal = inputs
        scores = jnp.dot(rows, vocab, preferred_element_type=jnp.float32) + vocab_bias
        top = lax.optimization_barrier(jnp.max(scores, axis=1))
        lse = top + jnp.log(lax.optimization_barrier(jnp.sum(jnp.exp(scores - top[:, None]), axis=1)))
        hit = lax.broadcasted_iota(jnp.int32, (TOK_GROUP, VOCAB), 1) == goal[:, None]
        target_score = lax.optimization_barrier(jnp.sum(jnp.where(hit, scores, 0.0), axis=1))
        losses = lse - target_score + zloss_weight * lse * lse
        probs = jnp.exp(scores - lse[:, None])
        dscore = (probs * (1.0 + 2.0 * zloss_weight * lse)[:, None] - jnp.where(hit, 1.0, 0.0)).astype(jnp.bfloat16)
        drows = jnp.dot(dscore, vocab.T, preferred_element_type=jnp.float32)
        carry = carry + jnp.dot(rows.T, dscore, preferred_element_type=jnp.float32)
        return (carry, (losses, drows))
    grad_vocab, (losses, drows) = lax.scan(one_group, jnp.zeros((D, VOCAB), jnp.float32), (normed_blocks, target_blocks))
    dnormed = drows.reshape(TOKENS, D)
    scaled = dnormed * final_gain
    grad_input = inv * (scaled - values * inv * inv * lax.optimization_barrier(jnp.mean(values * scaled, axis=1, keepdims=True)))
    return (losses.reshape(TOKENS), grad_input, grad_vocab)
```

```python
import functools

import jax
import jax.numpy as jnp
from jax import lax
from jax.experimental import pallas as pl
from jax.experimental.pallas import tpu as pltpu
from jax.sharding import PartitionSpec as P

norm_eps = 1e-06
zloss_weight = 0.001


def combined_all(value, axis, join):
    pieces = jax.tree.map(lambda part: lax.all_gather(part, axis), value)
    head = jax.tree.map(lambda part: part[0], pieces)
    tail = jax.tree.map(lambda part: part[1:], pieces)
    total, _ = lax.scan(lambda total, section: (join(total, section), None), head, tail)
    return total


def combine_stats(first, second):
    top = jnp.maximum(first[0], second[0])
    total = first[1] * jnp.exp(first[0] - top) + second[1] * jnp.exp(second[0] - top)
    return (top, total, first[2] + second[2])


def body(stream, hidden, w_down, final_gain, vocab, vocab_bias, targets):
    rows_dev = stream.shape[0]
    width = stream.shape[1]
    group = targets.shape[0]
    mine = lax.axis_index("vp")
    feat_cols = w_down.shape[1]
    proj = jnp.dot(
        lax.all_gather(hidden, "vp", axis=1, tiled=True), w_down, preferred_element_type=jnp.float32
    )
    stream_cols = lax.all_to_all(stream, "vp", split_axis=1, concat_axis=0, tiled=True)
    normin_cols = (stream_cols.astype(jnp.float32) + proj).astype(jnp.bfloat16)
    col_values = normin_cols.astype(jnp.float32)
    square_total = lax.psum(jnp.sum(col_values * col_values, axis=1), "vp")
    inv_group = lax.rsqrt(square_total / width + norm_eps)
    gain_cols = lax.dynamic_slice_in_dim(final_gain, mine * feat_cols, feat_cols)
    normed_cols = (col_values * inv_group[:, None] * gain_cols).astype(jnp.bfloat16)
    normed = lax.all_gather(normed_cols, "vp", axis=1, tiled=True)
    normin = lax.all_to_all(normin_cols, "vp", split_axis=0, concat_axis=1, tiled=True)
    values = normin.astype(jnp.float32)
    inv = lax.rsqrt(jnp.mean(values * values, axis=1, keepdims=True) + norm_eps)
    ncols = vocab.shape[1]
    scores = jnp.dot(normed, vocab, preferred_element_type=jnp.float32) + vocab_bias
    local_top = jnp.max(scores, axis=1)
    local_total = jnp.sum(jnp.exp(scores - local_top[:, None]), axis=1)
    column_ids = lax.broadcasted_iota(jnp.int32, (group, ncols), 1) + mine * ncols
    hit = column_ids == targets[:, None]
    local_target = jnp.sum(jnp.where(hit, scores, 0.0), axis=1)
    top, total, target_score = combined_all(
        (local_top, local_total, local_target), "vp", combine_stats
    )
    lse = top + jnp.log(total)
    group_losses = lse - target_score + zloss_weight * lse * lse
    losses = lax.dynamic_slice_in_dim(group_losses, mine * rows_dev, rows_dev)
    probs = jnp.exp(scores - lse[:, None])
    dscore = (probs * (1.0 + 2.0 * zloss_weight * lse)[:, None] - jnp.where(hit, 1.0, 0.0)).astype(
        jnp.bfloat16
    )
    feat_group = width // lax.axis_size("dp")
    feat_start = lax.axis_index("dp") * feat_group
    rows_slice = lax.dynamic_slice_in_dim(
        lax.all_gather(normed, "dp", axis=0, tiled=True), feat_start, feat_group, 1
    )
    grad_vocab = lax.dot_general(
        rows_slice,
        lax.all_gather(dscore, "dp", axis=0, tiled=True),
        (((0,), (0,)), ((), ())),
        preferred_element_type=jnp.float32,
    )
    row_term = lax.dot_general(
        dscore, vocab, (((1,), (1,)), ((), ())), preferred_element_type=jnp.float32
    )
    row_parts = lax.all_to_all(
        row_term[:, None, :].astype(jnp.bfloat16), "vp", split_axis=0, concat_axis=1, tiled=True
    ).astype(jnp.float32)
    dnormed = jnp.sum(row_parts, axis=1)
    scaled = dnormed * final_gain
    grad_input = inv * (
        scaled - values * inv * inv * jnp.mean(values * scaled, axis=1, keepdims=True)
    )
    return (losses, grad_input, grad_vocab)


MESH = pl.DeviceIdType.MESH
HALVES = 2
TILE = 512


def send(src, dst, send_sem, recv_sem, vp, dp):
    return pltpu.make_async_remote_copy(
        src_ref=src,
        dst_ref=dst,
        send_sem=send_sem,
        recv_sem=recv_sem,
        device_id={"vp": vp, "dp": dp},
        device_id_type=MESH,
    )


def gather(n, me, dp, own, place, sems, extra):
    line = n // 2
    row = me // 2
    side = me - 2 * row
    other = me + 1 - 2 * side
    send_sem, recv_sem = sems

    def copy(way, slot, part, target, src=None):
        src = place(slot, part) if src is None else src
        return send(
            src,
            place(slot, part),
            send_sem.at[way, slot, part],
            recv_sem.at[slot, part],
            target,
            dp,
        )

    for part in range(HALVES):
        copy(0, me, part, other, own(part)).start()

        @pl.when(row < line - 1)
        def _():
            copy(1, me, part, me + 2, own(part)).start()

        @pl.when(row > 0)
        def _():
            copy(2, me, part, me - 2, own(part)).start()

        extra(me, part)

    def crossed(k):
        for part in range(HALVES):
            for step in (-k, k) if k else (0,):
                slot = other + 2 * step

                @pl.when((row + step >= 0) & (row + step < line))
                def _():
                    copy(0, slot, part, other).wait_recv()
                    extra(slot, part)

    for k in range(1, line):
        for part in range(HALVES):
            for step, way in ((-k, 1), (k, 2)):
                slot = me + 2 * step

                @pl.when((row + step >= 0) & (row + step < line))
                def _():
                    copy(0, slot, part, other).wait_recv()
                    on = row < line - 1 if way == 1 else row > 0

                    @pl.when(on)
                    def _():
                        copy(way, slot, part, me + 2 if way == 1 else me - 2).start()

                    copy(0, slot, part, other).start()
                    extra(slot, part)

        crossed(k - 1)
    crossed(line - 1)

    def finish():
        for part in range(HALVES):
            copy(0, me, part, other, own(part)).wait_send()

            @pl.when(row < line - 1)
            def _():
                copy(1, me, part, me + 2, own(part)).wait_send()

            @pl.when(row > 0)
            def _():
                copy(2, me, part, me - 2, own(part)).wait_send()

            for k in range(1, line):
                for step, way in ((-k, 1), (k, 2)):
                    slot = me + 2 * step

                    @pl.when((row + step >= 0) & (row + step < line))
                    def _():
                        copy(0, slot, part, other).wait_send()

                        @pl.when(row < line - 1 if way == 1 else row > 0)
                        def _():
                            copy(way, slot, part, me).wait_send()

    return finish


def head_kernel(
    n,
    hidden,
    w_down,
    stream,
    gain,
    vocab,
    bias,
    targets,
    loss_out,
    input_out,
    vocab_out,
    units,
    stream_cols,
    normin,
    normed,
    words,
    scores,
    tops,
    lanes,
    stats,
    dscore,
    slices,
    flipped,
    terms,
    landed,
    staged,
    unit_send,
    unit_recv,
    norm_send,
    norm_recv,
    stream_send,
    stream_recv,
    twin_send,
    twin_recv,
    stat_send,
    stat_recv,
    score_send,
    score_recv,
    slice_send,
    slice_recv,
    term_send,
    term_recv,
    load_sem,
    out_sem,
):
    me = lax.axis_index("vp")
    dp = lax.axis_index("dp")
    twin = lax.rem(dp + 2, 4)
    core = lax.rem(dp, 2)
    sibling = dp + 1 - 2 * core
    group, depth = hidden.shape
    width = gain.shape[1]
    feats = stream_cols.shape[1]
    rows_dev = stream.shape[0]
    ncols = bias.shape[1]
    own_feats = slices.shape[1]
    half = group // HALVES

    load = pltpu.make_async_copy(vocab, words, load_sem)
    load.start()
    barrier = pltpu.get_barrier_semaphore()

    def greet(j, _):
        peer = lax.rem(me + j, n)
        pl.semaphore_signal(barrier, 1, device_id={"vp": peer, "dp": dp}, device_id_type=MESH)
        pl.semaphore_signal(barrier, 1, device_id={"vp": peer, "dp": twin}, device_id_type=MESH)
        return 0

    lax.fori_loop(1, n, greet, 0)
    pl.semaphore_signal(barrier, 1, device_id={"vp": me, "dp": twin}, device_id_type=MESH)
    pl.semaphore_signal(barrier, 1, device_id={"vp": me, "dp": sibling}, device_id_type=MESH)
    pl.semaphore_wait(barrier, 2 * n)

    def stream_copy(j):
        peer = lax.rem(me + j, n)
        return send(
            stream.at[:, pl.ds(pl.multiple_of(peer * feats, 128), feats)],
            stream_cols.at[pl.ds(pl.multiple_of(me * rows_dev, rows_dev), rows_dev), :],
            stream_send.at[j],
            stream_recv.at[j],
            peer,
            dp,
        )

    def start_stream(j, _):
        stream_copy(j).start()
        return 0

    def wait_stream(j, _):
        stream_copy(j).wait()
        return 0

    units[me] = hidden[...]
    stream_cols[pl.ds(pl.multiple_of(me * rows_dev, rows_dev), rows_dev), :] = stream[
        :, pl.ds(pl.multiple_of(me * feats, 128), feats)
    ]
    lax.fori_loop(1, n, start_stream, 0)
    finish_units = gather(
        n,
        me,
        dp,
        lambda part: hidden.at[pl.ds(part * half, half), :],
        lambda slot, part: units.at[slot, pl.ds(part * half, half), :],
        (unit_send, unit_recv),
        lambda slot, part: None,
    )
    lax.fori_loop(1, n, wait_stream, 0)

    def project(slot, total):
        rows = pl.ds(pl.multiple_of(slot * depth, 16), depth)
        return total + jnp.dot(units[slot], w_down[rows, :], preferred_element_type=jnp.float32)

    proj = lax.fori_loop(0, n, project, jnp.zeros((group, feats), jnp.float32))

    def cols_of(slot):
        return pl.ds(pl.multiple_of(slot * feats, 128), feats)

    normin[0, :, cols_of(me)] = (stream_cols[...].astype(jnp.float32) + proj).astype(jnp.bfloat16)

    def twin_copy(slot, part):
        rows = pl.ds(part * half, half)
        return send(
            normin.at[0, rows, cols_of(slot)],
            normin.at[1, rows, cols_of(slot)],
            twin_send.at[slot, part],
            twin_recv.at[slot, part],
            me,
            twin,
        )

    finish_norm = gather(
        n,
        me,
        dp,
        lambda part: normin.at[0, pl.ds(part * half, half), cols_of(me)],
        lambda slot, part: normin.at[0, pl.ds(part * half, half), cols_of(slot)],
        (norm_send, norm_recv),
        lambda slot, part: twin_copy(slot, part).start(),
    )

    def normalize(which):
        def block(j, _):
            rows = pl.ds(pl.multiple_of(j * 32, 32), 32)
            values = normin[which, rows, :].astype(jnp.float32)
            inv = lax.rsqrt(jnp.mean(values * values, axis=1, keepdims=True) + norm_eps)
            normed[which, rows, :] = (values * inv * gain[...]).astype(jnp.bfloat16)
            return 0

        lax.fori_loop(0, group // 32, block, 0)

    def slice_copy(which, home):
        rows = pl.ds(pl.multiple_of(home * group, group), group)
        cols = pl.ds(pl.multiple_of(sibling * own_feats, 128), own_feats)
        return send(
            normed.at[which, :, cols],
            slices.at[rows, :],
            slice_send.at[which],
            slice_recv.at[which],
            me,
            sibling,
        )

    def folded(values, join):
        result = values[:, :128]
        for at in range(128, TILE, 128):
            result = join(result, values[:, at : at + 128])
        return result

    def score(which):
        tops[which] = jnp.full((group, 128), -jnp.inf, jnp.float32)

        def block(j, _):
            cols = pl.ds(pl.multiple_of(j * TILE, TILE), TILE)
            values = (
                jnp.dot(normed[which], words[:, cols], preferred_element_type=jnp.float32)
                + bias[:, cols]
            )
            scores[which, :, cols] = values
            tops[which] = jnp.maximum(tops[which], folded(values, jnp.maximum))
            return 0

        lax.fori_loop(0, ncols // TILE, block, 0)
        top = jnp.max(tops[which], axis=1, keepdims=True)
        tops[which] = jnp.broadcast_to(top, (group, 128))
        lanes[...] = jnp.zeros_like(lanes)

        def powers(j, _):
            cols = pl.ds(pl.multiple_of(j * TILE, TILE), TILE)
            values = scores[which, :, cols]
            if which == 0:
                ids = lax.broadcasted_iota(jnp.int32, (group, TILE), 1) + (me * ncols + j * TILE)
                hits = jnp.where(ids == targets[...], values, 0.0)
                lanes[1] += folded(hits, jnp.add)
            values = jnp.exp(values - top)
            scores[which, :, cols] = values
            if which == 0:
                lanes[0] += folded(values, jnp.add)
            return 0

        lax.fori_loop(0, ncols // TILE, powers, 0)
        return top

    def stat_copy(away, j, home):
        peer = lax.rem(me + j, n)
        return send(
            stats.at[0, me],
            stats.at[away, me],
            stat_send.at[away, j],
            stat_recv.at[away, j],
            peer,
            home,
        )

    normalize(0)
    load.wait()
    slice_copy(0, dp).start()
    top = score(0)
    lane = lax.broadcasted_iota(jnp.int32, (group, 128), 1)
    packed = jnp.where(
        lane == 0,
        top,
        jnp.where(
            lane == 1,
            jnp.sum(lanes[0], axis=1, keepdims=True),
            jnp.where(
                lane == 2,
                jnp.sum(lanes[1], axis=1, keepdims=True),
                jnp.where(lane == 3, targets[...].astype(jnp.float32), 0.0),
            ),
        ),
    )
    stats[0, me] = jnp.transpose(packed)[:8, :]

    def start_stats(j, _):
        stat_copy(0, j, dp).start()
        stat_copy(1, j, twin).start()
        return 0

    def wait_stats(j, _):
        stat_copy(0, j, dp).wait()
        stat_copy(1, j, twin).wait()
        return 0

    stat_copy(1, 0, twin).start()
    lax.fori_loop(1, n, start_stats, 0)

    for slot in range(n):
        for part in range(HALVES):
            twin_copy(slot, part).wait()
    normalize(1)
    slice_copy(1, twin).start()
    score(1)
    stat_copy(1, 0, twin).wait()
    lax.fori_loop(1, n, wait_stats, 0)

    def score_copy(which, home):
        rows = pl.ds(pl.multiple_of(home * group, group), group)
        return send(
            dscore.at[rows, :],
            dscore.at[rows, :],
            score_send.at[which],
            score_recv.at[which],
            me,
            sibling,
        )

    def derive(which, home):
        parts = stats[which]
        highest = jnp.max(parts[:, 0, :], axis=0, keepdims=True)
        total = jnp.sum(parts[:, 1, :] * jnp.exp(parts[:, 0, :] - highest), axis=0, keepdims=True)
        lse = highest + jnp.log(total)
        if which == 0:
            goal = jnp.sum(parts[:, 2, :], axis=0, keepdims=True)
            loss_out[...] = lse - goal + zloss_weight * lse * lse
        level = lax.broadcasted_iota(jnp.int32, (128, group), 0)
        turned = jnp.transpose(
            jnp.where(level == 0, lse, jnp.where(level == 1, parts[0, 3:4, :], 0.0))
        )
        lse_col = turned[:, 0:1]
        goal_col = turned[:, 1:2].astype(jnp.int32)
        factor = jnp.exp(tops[which][:, 0:1] - lse_col) * (1.0 + 2.0 * zloss_weight * lse_col)
        rows = pl.ds(pl.multiple_of(home * group, group), group)

        def block(j, _):
            cols = pl.ds(pl.multiple_of(j * TILE, TILE), TILE)
            ids = lax.broadcasted_iota(jnp.int32, (group, TILE), 1) + (me * ncols + j * TILE)
            values = scores[which, :, cols] * factor - jnp.where(ids == goal_col, 1.0, 0.0)
            dscore[rows, cols] = values.astype(jnp.bfloat16)
            return 0

        lax.fori_loop(0, ncols // TILE, block, 0)
        score_copy(which, home).start()

    derive(0, dp)
    derive(1, twin)

    def term_copy(t, j):
        peer = lax.rem(me + j, n)
        cols = pl.ds(pl.multiple_of(t * TILE, TILE), TILE)
        return send(
            terms.at[pl.ds(pl.multiple_of(peer * rows_dev, rows_dev), rows_dev), cols],
            landed.at[me, :, cols],
            term_send.at[t, j],
            term_recv.at[t, j],
            peer,
            dp,
        )

    own_rows = pl.ds(pl.multiple_of(dp * group, group), group)

    def term_block(t, _):
        cols = pl.ds(pl.multiple_of(t * TILE, TILE), TILE)
        terms[:, cols] = lax.dot_general(
            dscore[own_rows, :],
            words[cols, :],
            (((1,), (1,)), ((), ())),
            preferred_element_type=jnp.float32,
        ).astype(jnp.bfloat16)

        def start(j, _):
            term_copy(t, j).start()
            return 0

        return lax.fori_loop(1, n, start, 0)

    lax.fori_loop(0, width // TILE, term_block, 0)
    my_rows = pl.ds(pl.multiple_of(me * rows_dev, rows_dev), rows_dev)
    landed[me] = terms[my_rows, :]

    for which, home in ((0, dp), (1, twin)):
        rows = pl.ds(pl.multiple_of(home * group, group), group)
        slices[rows, :] = normed[which, :, pl.ds(pl.multiple_of(dp * own_feats, 128), own_feats)]
        slice_copy(which, home).wait()
        score_copy(which, home).wait()
    flipped[...] = jnp.transpose(slices[...])

    def out_copy(j):
        slot = lax.rem(j, 2)
        cols = pl.ds(pl.multiple_of(j * TILE, TILE), TILE)
        return pltpu.make_async_copy(staged.at[slot], vocab_out.at[:, cols], out_sem.at[slot])

    def vocab_block(j, _):
        @pl.when(j >= 2)
        def _():
            out_copy(j - 2).wait()

        cols = pl.ds(pl.multiple_of(j * TILE, TILE), TILE)
        staged[lax.rem(j, 2)] = jnp.dot(
            flipped[...], dscore[:, cols], preferred_element_type=jnp.float32
        )
        out_copy(j).start()
        return 0

    blocks = ncols // TILE
    lax.fori_loop(0, blocks, vocab_block, 0)

    def wait_terms(t, _):
        def wait(j, _):
            term_copy(t, j).wait()
            return 0

        return lax.fori_loop(1, n, wait, 0)

    lax.fori_loop(0, width // TILE, wait_terms, 0)
    values = normin[0, my_rows, :].astype(jnp.float32)
    inv = lax.rsqrt(jnp.mean(values * values, axis=1, keepdims=True) + norm_eps)
    dnormed = landed[0].astype(jnp.float32)
    for slot in range(1, n):
        dnormed += landed[slot].astype(jnp.float32)
    scaled = dnormed * gain[...]
    input_out[...] = inv * (
        scaled - values * inv * inv * jnp.mean(values * scaled, axis=1, keepdims=True)
    )
    for j in range(max(blocks - 2, 0), blocks):
        out_copy(j).wait()
    finish_units()
    finish_norm()


def fused(stream, hidden, w_down, final_gain, vocab, vocab_bias, targets):
    n = lax.axis_size("vp")
    groups = lax.axis_size("dp")
    rows_dev, width = stream.shape
    group, depth = hidden.shape
    feats = w_down.shape[1]
    ncols = vocab.shape[1]
    own_feats = width // groups
    f32, bf16 = jnp.float32, jnp.bfloat16
    dma = pltpu.SemaphoreType.DMA
    vmem = pl.BlockSpec(memory_space=pltpu.VMEM)
    hbm = pl.BlockSpec(memory_space=pl.ANY)
    group_losses, grad_input, grad_vocab = pl.pallas_call(
        functools.partial(head_kernel, n),
        out_shape=(
            jax.ShapeDtypeStruct((1, group), f32),
            jax.ShapeDtypeStruct((rows_dev, width), f32),
            jax.ShapeDtypeStruct((own_feats, ncols), f32),
        ),
        in_specs=[vmem, vmem, vmem, vmem, hbm, vmem, vmem],
        out_specs=(vmem, vmem, hbm),
        scratch_shapes=[
            pltpu.VMEM((n, group, depth), bf16),
            pltpu.VMEM((group, feats), bf16),
            pltpu.VMEM((2, group, width), bf16),
            pltpu.VMEM((2, group, width), bf16),
            pltpu.VMEM((width, ncols), bf16),
            pltpu.VMEM((2, group, ncols), f32),
            pltpu.VMEM((2, group, 128), f32),
            pltpu.VMEM((2, group, 128), f32),
            pltpu.VMEM((2, n, 8, group), f32),
            pltpu.VMEM((groups * group, ncols), bf16),
            pltpu.VMEM((groups * group, own_feats), bf16),
            pltpu.VMEM((own_feats, groups * group), bf16),
            pltpu.VMEM((group, width), bf16),
            pltpu.VMEM((n, rows_dev, width), bf16),
            pltpu.VMEM((2, own_feats, TILE), f32),
            dma((3, n, HALVES)),
            dma((n, HALVES)),
            dma((3, n, HALVES)),
            dma((n, HALVES)),
            dma((n,)),
            dma((n,)),
            dma((n, HALVES)),
            dma((n, HALVES)),
            dma((2, n)),
            dma((2, n)),
            dma((2,)),
            dma((2,)),
            dma((2,)),
            dma((2,)),
            dma((width // TILE, n)),
            dma((width // TILE, n)),
            dma,
            dma((2,)),
        ],
        compiler_params=pltpu.CompilerParams(
            collective_id=0, has_side_effects=True, vmem_limit_bytes=64 * 1024 * 1024 - 65536
        ),
    )(
        hidden,
        w_down,
        stream,
        final_gain.reshape(1, width),
        vocab,
        vocab_bias.reshape(1, ncols),
        targets.reshape(group, 1),
    )
    losses = lax.dynamic_slice_in_dim(
        group_losses.reshape(group), lax.axis_index("vp") * rows_dev, rows_dev
    )
    return (losses, grad_input, grad_vocab)


def choose(stream, hidden, w_down, final_gain, vocab, vocab_bias, targets):
    rows_dev, width = stream.shape
    group, depth = hidden.shape
    n, groups = lax.axis_size("vp"), lax.axis_size("dp")
    tiles = (
        n % 2 == 0
        and groups == 4
        and rows_dev % 32 == 0
        and depth % 16 == 0
        and group % (32 * HALVES) == 0
        and w_down.shape[1] % 128 == 0
        and width % TILE == 0
        and (width // groups) % 128 == 0
        and vocab.shape[1] % TILE == 0
    )
    path = fused if tiles else body
    return path(stream, hidden, w_down, final_gain, vocab, vocab_bias, targets)


def solution(mesh):
    placed = (
        P(("dp", "vp"), None),
        P("dp", "vp"),
        P(None, "vp"),
        P(),
        P(None, "vp"),
        P("vp"),
        P("dp"),
    )
    return jax.shard_map(
        choose,
        mesh=mesh,
        in_specs=placed,
        out_specs=(P(("dp", "vp")), P(("dp", "vp"), None), P("dp", "vp")),
        check_vma=False,
    )
```

```python
import functools

import jax
import jax.numpy as jnp
from jax import lax
from jax.experimental import pallas as pl
from jax.experimental.pallas import tpu as pltpu
from jax.sharding import PartitionSpec as P

norm_eps = 1e-06
zloss_weight = 0.001


def combined_all(value, axis, join):
    pieces = jax.tree.map(lambda part: lax.all_gather(part, axis), value)
    head = jax.tree.map(lambda part: part[0], pieces)
    tail = jax.tree.map(lambda part: part[1:], pieces)
    total, _ = lax.scan(lambda total, section: (join(total, section), None), head, tail)
    return total


def combine_stats(first, second):
    top = jnp.maximum(first[0], second[0])
    total = first[1] * jnp.exp(first[0] - top) + second[1] * jnp.exp(second[0] - top)
    return (top, total, first[2] + second[2])


def body(stream, hidden, w_down, final_gain, vocab, vocab_bias, targets):
    rows_dev = stream.shape[0]
    width = stream.shape[1]
    group = targets.shape[0]
    mine = lax.axis_index("vp")
    feat_cols = w_down.shape[1]
    proj = jnp.dot(
        lax.all_gather(hidden, "vp", axis=1, tiled=True), w_down, preferred_element_type=jnp.float32
    )
    stream_cols = lax.all_to_all(stream, "vp", split_axis=1, concat_axis=0, tiled=True)
    normin_cols = (stream_cols.astype(jnp.float32) + proj).astype(jnp.bfloat16)
    col_values = normin_cols.astype(jnp.float32)
    square_total = lax.psum(jnp.sum(col_values * col_values, axis=1), "vp")
    inv_group = lax.rsqrt(square_total / width + norm_eps)
    gain_cols = lax.dynamic_slice_in_dim(final_gain, mine * feat_cols, feat_cols)
    normed_cols = (col_values * inv_group[:, None] * gain_cols).astype(jnp.bfloat16)
    normed = lax.all_gather(normed_cols, "vp", axis=1, tiled=True)
    normin = lax.all_to_all(normin_cols, "vp", split_axis=0, concat_axis=1, tiled=True)
    values = normin.astype(jnp.float32)
    inv = lax.rsqrt(jnp.mean(values * values, axis=1, keepdims=True) + norm_eps)
    ncols = vocab.shape[1]
    scores = jnp.dot(normed, vocab, preferred_element_type=jnp.float32) + vocab_bias
    local_top = jnp.max(scores, axis=1)
    local_total = jnp.sum(jnp.exp(scores - local_top[:, None]), axis=1)
    column_ids = lax.broadcasted_iota(jnp.int32, (group, ncols), 1) + mine * ncols
    hit = column_ids == targets[:, None]
    local_target = jnp.sum(jnp.where(hit, scores, 0.0), axis=1)
    top, total, target_score = combined_all(
        (local_top, local_total, local_target), "vp", combine_stats
    )
    lse = top + jnp.log(total)
    group_losses = lse - target_score + zloss_weight * lse * lse
    losses = lax.dynamic_slice_in_dim(group_losses, mine * rows_dev, rows_dev)
    probs = jnp.exp(scores - lse[:, None])
    dscore = (probs * (1.0 + 2.0 * zloss_weight * lse)[:, None] - jnp.where(hit, 1.0, 0.0)).astype(
        jnp.bfloat16
    )
    feat_group = width // lax.axis_size("dp")
    feat_start = lax.axis_index("dp") * feat_group
    rows_slice = lax.dynamic_slice_in_dim(
        lax.all_gather(normed, "dp", axis=0, tiled=True), feat_start, feat_group, 1
    )
    grad_vocab = lax.dot_general(
        rows_slice,
        lax.all_gather(dscore, "dp", axis=0, tiled=True),
        (((0,), (0,)), ((), ())),
        preferred_element_type=jnp.float32,
    )
    row_term = lax.dot_general(
        dscore, vocab, (((1,), (1,)), ((), ())), preferred_element_type=jnp.float32
    )
    row_parts = lax.all_to_all(
        row_term[:, None, :].astype(jnp.bfloat16), "vp", split_axis=0, concat_axis=1, tiled=True
    ).astype(jnp.float32)
    dnormed = jnp.sum(row_parts, axis=1)
    scaled = dnormed * final_gain
    grad_input = inv * (
        scaled - values * inv * inv * jnp.mean(values * scaled, axis=1, keepdims=True)
    )
    return (losses, grad_input, grad_vocab)


MESH = pl.DeviceIdType.MESH
HALVES = 2
TILE = 512


def send(src, dst, send_sem, recv_sem, vp, dp):
    return pltpu.make_async_remote_copy(
        src_ref=src,
        dst_ref=dst,
        send_sem=send_sem,
        recv_sem=recv_sem,
        device_id={"vp": vp, "dp": dp},
        device_id_type=MESH,
    )


def gather(n, me, dp, own, place, sems, extra, use):
    line = n // 2
    row = me // 2
    side = me - 2 * row
    other = me + 1 - 2 * side
    send_sem, recv_sem = sems

    def copy(way, slot, part, target, src=None):
        src = place(slot, part) if src is None else src
        return send(
            src,
            place(slot, part),
            send_sem.at[way, slot, part],
            recv_sem.at[slot, part],
            target,
            dp,
        )

    for part in range(HALVES):
        copy(0, me, part, other, own(part)).start()

        @pl.when(row < line - 1)
        def _():
            copy(1, me, part, me + 2, own(part)).start()

        @pl.when(row > 0)
        def _():
            copy(2, me, part, me - 2, own(part)).start()

        extra(me, part)
    use(me)

    def crossed(k):
        for part in range(HALVES):
            for step in (-k, k) if k else (0,):
                slot = other + 2 * step

                @pl.when((row + step >= 0) & (row + step < line))
                def _():
                    copy(0, slot, part, other).wait_recv()
                    extra(slot, part)

    def used(k):
        for step in (-k, k) if k else (0,):

            @pl.when((row + step >= 0) & (row + step < line))
            def _():
                use(other + 2 * step)

    for k in range(1, line):
        for part in range(HALVES):
            for step, way in ((-k, 1), (k, 2)):
                slot = me + 2 * step

                @pl.when((row + step >= 0) & (row + step < line))
                def _():
                    copy(0, slot, part, other).wait_recv()
                    on = row < line - 1 if way == 1 else row > 0

                    @pl.when(on)
                    def _():
                        copy(way, slot, part, me + 2 if way == 1 else me - 2).start()

                    copy(0, slot, part, other).start()
                    extra(slot, part)

        crossed(k - 1)
        for step in (-k, k):

            @pl.when((row + step >= 0) & (row + step < line))
            def _():
                use(me + 2 * step)

        used(k - 1)
    crossed(line - 1)
    used(line - 1)

    def finish():
        for part in range(HALVES):
            copy(0, me, part, other, own(part)).wait_send()

            @pl.when(row < line - 1)
            def _():
                copy(1, me, part, me + 2, own(part)).wait_send()

            @pl.when(row > 0)
            def _():
                copy(2, me, part, me - 2, own(part)).wait_send()

            for k in range(1, line):
                for step, way in ((-k, 1), (k, 2)):
                    slot = me + 2 * step

                    @pl.when((row + step >= 0) & (row + step < line))
                    def _():
                        copy(0, slot, part, other).wait_send()

                        @pl.when(row < line - 1 if way == 1 else row > 0)
                        def _():
                            copy(way, slot, part, me).wait_send()

    return finish


def head_kernel(
    n,
    hidden,
    w_down,
    stream,
    gain,
    vocab,
    bias,
    targets,
    loss_out,
    input_out,
    score_out,
    flip_out,
    units,
    stream_cols,
    normin,
    normed,
    words,
    scores,
    tops,
    lanes,
    stats,
    goals,
    total,
    dscore,
    slices,
    terms,
    landed,
    unit_send,
    unit_recv,
    norm_send,
    norm_recv,
    stream_send,
    stream_recv,
    twin_send,
    twin_recv,
    stat_send,
    stat_recv,
    score_send,
    score_recv,
    slice_send,
    slice_recv,
    term_send,
    term_recv,
    load_sem,
    unit_sem,
    out_sem,
):
    me = lax.axis_index("vp")
    dp = lax.axis_index("dp")
    twin = lax.rem(dp + 2, 4)
    core = lax.rem(dp, 2)
    sibling = dp + 1 - 2 * core
    depth, group = hidden.shape
    width = gain.shape[1]
    feats = stream_cols.shape[1]
    rows_dev = stream.shape[0]
    ncols = bias.shape[1]
    own_feats = slices.shape[1]
    half = group // HALVES
    piece = depth // HALVES

    load = pltpu.make_async_copy(vocab, words, load_sem)
    bring = pltpu.make_async_copy(hidden, units.at[me], unit_sem)
    bring.start()
    load.start()
    goals[...] = jnp.transpose(jnp.broadcast_to(targets[...].astype(jnp.float32), (128, group)))
    total[...] = jnp.zeros_like(total)
    barrier = pltpu.get_barrier_semaphore()

    def greet(j, _):
        peer = lax.rem(me + j, n)
        pl.semaphore_signal(barrier, 1, device_id={"vp": peer, "dp": dp}, device_id_type=MESH)
        pl.semaphore_signal(barrier, 1, device_id={"vp": peer, "dp": twin}, device_id_type=MESH)
        return 0

    lax.fori_loop(1, n, greet, 0)
    pl.semaphore_signal(barrier, 1, device_id={"vp": me, "dp": twin}, device_id_type=MESH)
    pl.semaphore_signal(barrier, 1, device_id={"vp": me, "dp": sibling}, device_id_type=MESH)
    pl.semaphore_wait(barrier, 2 * n)

    def stream_copy(j):
        peer = lax.rem(me + j, n)
        return send(
            stream.at[:, pl.ds(pl.multiple_of(peer * feats, 128), feats)],
            stream_cols.at[pl.ds(pl.multiple_of(me * rows_dev, rows_dev), rows_dev), :],
            stream_send.at[j],
            stream_recv.at[j],
            peer,
            dp,
        )

    def start_stream(j, _):
        stream_copy(j).start()
        return 0

    def wait_stream(j, _):
        stream_copy(j).wait()
        return 0

    bring.wait()
    stream_cols[pl.ds(pl.multiple_of(me * rows_dev, rows_dev), rows_dev), :] = stream[
        :, pl.ds(pl.multiple_of(me * feats, 128), feats)
    ]
    lax.fori_loop(1, n, start_stream, 0)
    def place_units(slot, part):
        return units.at[slot, pl.ds(part * piece, piece), :]

    def project(slot):
        rows = pl.ds(pl.multiple_of(slot * depth, 16), depth)
        total[...] += lax.dot_general(
            units[slot],
            w_down[rows, :],
            (((0,), (0,)), ((), ())),
            preferred_element_type=jnp.float32,
        )

    finish_units = gather(
        n,
        me,
        dp,
        lambda part: place_units(me, part),
        place_units,
        (unit_send, unit_recv),
        lambda slot, part: None,
        project,
    )
    lax.fori_loop(1, n, wait_stream, 0)

    def cols_of(slot):
        return pl.ds(pl.multiple_of(slot * feats, 128), feats)

    normin[0, :, cols_of(me)] = (stream_cols[...].astype(jnp.float32) + total[...]).astype(jnp.bfloat16)

    def twin_copy(slot, part):
        rows = pl.ds(part * half, half)
        return send(
            normin.at[0, rows, cols_of(slot)],
            normin.at[1, rows, cols_of(slot)],
            twin_send.at[slot, part],
            twin_recv.at[slot, part],
            me,
            twin,
        )

    finish_norm = gather(
        n,
        me,
        dp,
        lambda part: normin.at[0, pl.ds(part * half, half), cols_of(me)],
        lambda slot, part: normin.at[0, pl.ds(part * half, half), cols_of(slot)],
        (norm_send, norm_recv),
        lambda slot, part: twin_copy(slot, part).start(),
        lambda slot: None,
    )

    def normalize(which):
        def block(j, _):
            rows = pl.ds(pl.multiple_of(j * 32, 32), 32)
            values = normin[which, rows, :].astype(jnp.float32)
            inv = lax.rsqrt(jnp.mean(values * values, axis=1, keepdims=True) + norm_eps)
            normed[which, rows, :] = (values * inv * gain[...]).astype(jnp.bfloat16)
            return 0

        lax.fori_loop(0, group // 32, block, 0)

    def slice_copy(which, home):
        rows = pl.ds(pl.multiple_of(home * group, group), group)
        cols = pl.ds(pl.multiple_of(sibling * own_feats, 128), own_feats)
        return send(
            normed.at[which, :, cols],
            slices.at[rows, :],
            slice_send.at[which],
            slice_recv.at[which],
            me,
            sibling,
        )

    def folded(values, join):
        result = values[:, :128]
        for at in range(128, TILE, 128):
            result = join(result, values[:, at : at + 128])
        return result

    def score(which, first, last):
        def block(j, _):
            cols = pl.ds(pl.multiple_of(j * TILE, TILE), TILE)
            values = (
                jnp.dot(normed[which], words[:, cols], preferred_element_type=jnp.float32)
                + bias[:, cols]
            )
            scores[which, :, cols] = values
            tops[which] = jnp.maximum(tops[which], folded(values, jnp.maximum))
            return 0

        lax.fori_loop(first, last, block, 0)

    def level(which):
        top = jnp.max(tops[which], axis=1, keepdims=True)
        tops[which] = jnp.broadcast_to(top, (group, 128))
        lanes[...] = jnp.zeros_like(lanes)

        def powers(j, _):
            cols = pl.ds(pl.multiple_of(j * TILE, TILE), TILE)
            values = scores[which, :, cols]
            if which == 0:
                ids = lax.broadcasted_iota(jnp.int32, (group, TILE), 1) + (me * ncols + j * TILE)
                hits = jnp.where(ids == own_goals, values, 0.0)
                lanes[1] += folded(hits, jnp.add)
            values = jnp.exp(values - top)
            scores[which, :, cols] = values
            if which == 0:
                lanes[0] += folded(values, jnp.add)
            return 0

        lax.fori_loop(0, ncols // TILE, powers, 0)
        return top

    def stat_copy(away, j, home):
        peer = lax.rem(me + j, n)
        return send(
            stats.at[0, me],
            stats.at[away, me],
            stat_send.at[away, j],
            stat_recv.at[away, j],
            peer,
            home,
        )

    tops[...] = jnp.full(tops.shape, -jnp.inf, jnp.float32)
    own_goals = goals[:, 0:1].astype(jnp.int32)
    blocks = ncols // TILE
    middle = blocks // 2
    normalize(0)
    load.wait()
    slice_copy(0, dp).start()
    score(0, 0, blocks)
    top = level(0)
    lane = lax.broadcasted_iota(jnp.int32, (group, 128), 1)
    packed = jnp.where(
        lane == 0,
        top,
        jnp.where(
            lane == 1,
            jnp.sum(lanes[0], axis=1, keepdims=True),
            jnp.where(
                lane == 2,
                jnp.sum(lanes[1], axis=1, keepdims=True),
                jnp.where(lane == 3, goals[...], 0.0),
            ),
        ),
    )
    stats[0, me] = jnp.transpose(packed)[:8, :]

    def start_stats(j, _):
        stat_copy(0, j, dp).start()
        stat_copy(1, j, twin).start()
        return 0

    stat_copy(1, 0, twin).start()
    lax.fori_loop(1, n, start_stats, 0)

    for slot in range(n):
        for part in range(HALVES):
            twin_copy(slot, part).wait()
    normalize(1)
    slice_copy(1, twin).start()
    score(1, 0, middle)

    def wait_stats(away, home):
        def wait(j, _):
            stat_copy(away, j, home).wait()
            return 0

        lax.fori_loop(1, n, wait, 0)

    def score_copy(which, home):
        rows = pl.ds(pl.multiple_of(home * group, group), group)
        return send(
            dscore.at[which],
            score_out.at[rows, :],
            score_send.at[which],
            score_recv.at[which],
            me,
            sibling,
        )

    def keep_copy(which, home):
        rows = pl.ds(pl.multiple_of(home * group, group), group)
        return pltpu.make_async_copy(dscore.at[which], score_out.at[rows, :], out_sem.at[which])

    def derive(which, home):
        parts = stats[which]
        highest = jnp.max(parts[:, 0, :], axis=0, keepdims=True)
        total = jnp.sum(parts[:, 1, :] * jnp.exp(parts[:, 0, :] - highest), axis=0, keepdims=True)
        lse = highest + jnp.log(total)
        if which == 0:
            goal = jnp.sum(parts[:, 2, :], axis=0, keepdims=True)
            loss_out[...] = jnp.broadcast_to(lse - goal + zloss_weight * lse * lse, (8, group))
        line = lax.broadcasted_iota(jnp.int32, (128, group), 0)
        turned = jnp.transpose(
            jnp.where(line == 0, lse, jnp.where(line == 1, parts[0, 3:4, :], 0.0))
        )
        lse_col = turned[:, 0:1]
        goal_col = turned[:, 1:2].astype(jnp.int32)
        factor = jnp.exp(tops[which][:, 0:1] - lse_col) * (1.0 + 2.0 * zloss_weight * lse_col)

        def block(j, _):
            cols = pl.ds(pl.multiple_of(j * TILE, TILE), TILE)
            ids = lax.broadcasted_iota(jnp.int32, (group, TILE), 1) + (me * ncols + j * TILE)
            values = scores[which, :, cols] * factor - jnp.where(ids == goal_col, 1.0, 0.0)
            dscore[which, :, cols] = values.astype(jnp.bfloat16)
            return 0

        lax.fori_loop(0, ncols // TILE, block, 0)
        score_copy(which, home).start()
        keep_copy(which, home).start()

    wait_stats(0, dp)
    derive(0, dp)

    def term_copy(t, j):
        peer = lax.rem(me + j, n)
        cols = pl.ds(pl.multiple_of(t * TILE, TILE), TILE)
        return send(
            terms.at[pl.ds(pl.multiple_of(peer * rows_dev, rows_dev), rows_dev), cols],
            landed.at[me, :, cols],
            term_send.at[t, j],
            term_recv.at[t, j],
            peer,
            dp,
        )

    def term_block(t, _):
        cols = pl.ds(pl.multiple_of(t * TILE, TILE), TILE)
        terms[:, cols] = lax.dot_general(
            dscore[0],
            words[cols, :],
            (((1,), (1,)), ((), ())),
            preferred_element_type=jnp.float32,
        ).astype(jnp.bfloat16)

        def start(j, _):
            term_copy(t, j).start()
            return 0

        return lax.fori_loop(1, n, start, 0)

    lax.fori_loop(0, width // TILE, term_block, 0)
    my_rows = pl.ds(pl.multiple_of(me * rows_dev, rows_dev), rows_dev)
    landed[me] = terms[my_rows, :]
    score(1, middle, blocks)
    level(1)
    stat_copy(1, 0, twin).wait()
    wait_stats(1, twin)
    derive(1, twin)

    for which, home in ((0, dp), (1, twin)):
        rows = pl.ds(pl.multiple_of(home * group, group), group)
        slices[rows, :] = normed[which, :, pl.ds(pl.multiple_of(dp * own_feats, 128), own_feats)]
        slice_copy(which, home).wait()
    flip_out[...] = jnp.transpose(slices[...])

    def wait_terms(t, _):
        def wait(j, _):
            term_copy(t, j).wait()
            return 0

        return lax.fori_loop(1, n, wait, 0)

    lax.fori_loop(0, width // TILE, wait_terms, 0)
    values = normin[0, my_rows, :].astype(jnp.float32)
    inv = lax.rsqrt(jnp.mean(values * values, axis=1, keepdims=True) + norm_eps)
    dnormed = landed[0].astype(jnp.float32)
    for slot in range(1, n):
        dnormed += landed[slot].astype(jnp.float32)
    scaled = dnormed * gain[...]
    input_out[...] = inv * (
        scaled - values * inv * inv * jnp.mean(values * scaled, axis=1, keepdims=True)
    )
    for which, home in ((0, dp), (1, twin)):
        keep_copy(which, home).wait()
        score_copy(which, home).wait()
    finish_units()
    finish_norm()


def vocab_kernel(flipped, dscore, grad_input, losses, vocab_out, input_out, loss_out):
    rows_dev = loss_out.shape[1]
    group = losses.shape[1]
    vocab_out[...] = jnp.dot(flipped[...], dscore[...], preferred_element_type=jnp.float32)

    @pl.when(pl.program_id(0) == 0)
    def _():
        input_out[...] = grad_input[...]
        shift = lax.rem(group - lax.axis_index("vp") * rows_dev, group)
        loss_out[...] = pltpu.roll(losses[...], shift, 1)[0:1, :rows_dev]


def fused(stream, hidden, w_down, final_gain, vocab, vocab_bias, targets):
    n = lax.axis_size("vp")
    groups = lax.axis_size("dp")
    rows_dev, width = stream.shape
    group, depth = hidden.shape
    feats = w_down.shape[1]
    ncols = vocab.shape[1]
    own_feats = width // groups
    tokens = groups * group
    f32, bf16 = jnp.float32, jnp.bfloat16
    dma = pltpu.SemaphoreType.DMA
    vmem = pl.BlockSpec(memory_space=pltpu.VMEM)
    hbm = pl.BlockSpec(memory_space=pl.ANY)
    group_losses, grad_input, dscore, flipped = pl.pallas_call(
        functools.partial(head_kernel, n),
        out_shape=(
            jax.ShapeDtypeStruct((8, group), f32),
            jax.ShapeDtypeStruct((rows_dev, width), f32),
            jax.ShapeDtypeStruct((tokens, ncols), bf16),
            jax.ShapeDtypeStruct((own_feats, tokens), bf16),
        ),
        in_specs=[hbm, vmem, vmem, vmem, hbm, vmem, vmem],
        out_specs=(vmem, vmem, hbm, vmem),
        scratch_shapes=[
            pltpu.VMEM((n, depth, group), bf16),
            pltpu.VMEM((group, feats), bf16),
            pltpu.VMEM((2, group, width), bf16),
            pltpu.VMEM((2, group, width), bf16),
            pltpu.VMEM((width, ncols), bf16),
            pltpu.VMEM((2, group, ncols), f32),
            pltpu.VMEM((2, group, 128), f32),
            pltpu.VMEM((2, group, 128), f32),
            pltpu.VMEM((2, n, 8, group), f32),
            pltpu.VMEM((group, 128), f32),
            pltpu.VMEM((group, feats), f32),
            pltpu.VMEM((2, group, ncols), bf16),
            pltpu.VMEM((tokens, own_feats), bf16),
            pltpu.VMEM((group, width), bf16),
            pltpu.VMEM((n, rows_dev, width), bf16),
            dma((3, n, HALVES)),
            dma((n, HALVES)),
            dma((3, n, HALVES)),
            dma((n, HALVES)),
            dma((n,)),
            dma((n,)),
            dma((n, HALVES)),
            dma((n, HALVES)),
            dma((2, n)),
            dma((2, n)),
            dma((2,)),
            dma((2,)),
            dma((2,)),
            dma((2,)),
            dma((width // TILE, n)),
            dma((width // TILE, n)),
            dma,
            dma,
            dma((2,)),
        ],
        compiler_params=pltpu.CompilerParams(
            collective_id=0, has_side_effects=True, vmem_limit_bytes=64 * 1024 * 1024 - 65536
        ),
    )(
        hidden.T,
        w_down,
        stream,
        final_gain.reshape(1, width),
        vocab,
        vocab_bias.reshape(1, ncols),
        targets.reshape(1, group),
    )

    def whole(*shape):
        return pl.BlockSpec(shape, lambda j: (0, 0))

    grad_vocab, grad_input, losses = pl.pallas_call(
        vocab_kernel,
        grid=(ncols // TILE,),
        out_shape=(
            jax.ShapeDtypeStruct((own_feats, ncols), f32),
            jax.ShapeDtypeStruct((rows_dev, width), f32),
            jax.ShapeDtypeStruct((1, rows_dev), f32),
        ),
        in_specs=[
            whole(own_feats, tokens),
            pl.BlockSpec((tokens, TILE), lambda j: (0, j)),
            whole(rows_dev, width),
            whole(8, group),
        ],
        out_specs=(
            pl.BlockSpec((own_feats, TILE), lambda j: (0, j)),
            whole(rows_dev, width),
            whole(1, rows_dev),
        ),
    )(flipped, dscore, grad_input, group_losses)
    return (losses.reshape(rows_dev), grad_input, grad_vocab)


def choose(stream, hidden, w_down, final_gain, vocab, vocab_bias, targets):
    rows_dev, width = stream.shape
    group, depth = hidden.shape
    n, groups = lax.axis_size("vp"), lax.axis_size("dp")
    tiles = (
        n % 2 == 0
        and groups == 4
        and rows_dev % 32 == 0
        and depth % (16 * HALVES) == 0
        and group % (32 * HALVES) == 0
        and w_down.shape[1] % 128 == 0
        and width % TILE == 0
        and (width // groups) % 128 == 0
        and vocab.shape[1] % TILE == 0
    )
    path = fused if tiles else body
    return path(stream, hidden, w_down, final_gain, vocab, vocab_bias, targets)


def solution(mesh):
    placed = (
        P(("dp", "vp"), None),
        P("dp", "vp"),
        P(None, "vp"),
        P(),
        P(None, "vp"),
        P("vp"),
        P("dp"),
    )
    return jax.shard_map(
        choose,
        mesh=mesh,
        in_specs=placed,
        out_specs=(P(("dp", "vp")), P(("dp", "vp"), None), P("dp", "vp")),
        check_vma=False,
    )
```
